32 devices in a mesh: tp: 8 (over z, x), dp: 4 (over y, core).
Axes of the slice: x: 2, y: 2, z: 4, core: 2. Of those that a mesh axis runs over, the one named last changes fastest.
Arguments:
- tokens: bfloat16 [112, 4096], P('tp', 'dp'), may hold values from -6 to 6
- w_query: bfloat16 [2, 4096, 4096], P(None, 'dp', 'tp'), may hold values from -0.09375 to 0.09375
- w_key: bfloat16 [2, 4096, 4096], P(None, 'dp', 'tp'), may hold values from -0.09375 to 0.09375
- w_value: bfloat16 [2, 4096, 4096], P(None, 'dp', 'tp'), may hold values from -0.09375 to 0.09375
- w_outgate: bfloat16 [2, 4096, 4096], P(None, 'dp', 'tp'), may hold values from -0.09375 to 0.09375
- w_ingate: bfloat16 [2, 4096, 32], P(None, 'dp'), may hold values from -0.09375 to 0.09375
- w_forget: bfloat16 [2, 4096, 32], P(None, 'dp'), may hold values from -0.09375 to 0.09375
- forget_bias: float32 [2, 32], P(None, 'tp'), may hold values from -2 to 3
- head_gain: float32 [2, 32, 128], P(None, 'tp'), may hold values from 0.1 to 1.9
- w_proj: bfloat16 [2, 4096, 4096], P(None, 'tp', 'dp'), may hold values from -0.09375 to 0.09375
- mem_matrix: float32 [2, 112, 32, 128, 128], P(None, 'dp', 'tp'), may hold values from -0.8 to 0.8
- mem_norm: float32 [2, 112, 32, 128], P(None, 'dp', 'tp'), may hold values from -1.2 to 1.2
- mem_max: float32 [2, 112, 32], P(None, 'dp', 'tp'), may hold values from -4 to 4
Outputs:
- result: bfloat16 [112, 4096], P('tp', 'dp')
- new_matrix: float32 [2, 112, 32, 128, 128], P(None, 'dp', 'tp')
- new_norm: float32 [2, 112, 32, 128], P(None, 'dp', 'tp')
- new_max: float32 [2, 112, 32], P(None, 'dp', 'tp')
The draws below stay inside these ranges and needn't reach their ends.
All inputs are finite; a program needn't handle non-finite values.
Results may differ from the reference program's by a relative error of at most 0.017.
Values may be sent and summed in bfloat16 or wider, within the bound.
A program may use at most 128 MiB of HBM per device.

```python
import jax
import jax.numpy as jnp
from jax import lax

D = 4096
HEADS = 32
HEAD = 128
BLOCKS = 2
BATCH = 112


def level_of(key, shape, pieces, low, largest):
    def one(position, blocks):
        draws = jax.random.uniform(jax.random.fold_in(jax.random.fold_in(key, 6), position), (blocks,), jnp.float32, low / len(pieces), largest / len(pieces))
        return jnp.repeat(jnp.exp(draws), shape[position] // blocks).reshape((-1,) + (1,) * (len(shape) - position - 1))

    loudness = one(*pieces[0])
    for cut in pieces[1:]:
        loudness = loudness * one(*cut)
    return loudness


def gaussian(stream_key, shape, deviation, limit, cuts=(), held_as=jnp.bfloat16):
    level = level_of(stream_key, shape, cuts, -0.22, 0.18) if cuts else 1.0
    array = jax.random.normal(stream_key, shape, jnp.float32) * deviation * level
    return jnp.minimum(jnp.maximum(array, -limit), limit).astype(held_as)


def setup_inputs(seed: int = 0) -> dict:
    keys = jax.random.split(jax.random.key(seed), 14)
    return {
        "tokens": gaussian(keys[0], (BATCH, D), 1.0, 6.0, ((0, 8), (1, 4))),
        "w_query": gaussian(keys[1], (BLOCKS, D, D), D ** -0.5, 0.09375, ((1, 4), (2, 8))),
        "w_key": gaussian(keys[2], (BLOCKS, D, D), D ** -0.5, 0.09375, ((1, 4), (2, 8))),
        "w_value": gaussian(keys[3], (BLOCKS, D, D), D ** -0.5, 0.09375, ((1, 4), (2, 8))),
        "w_outgate": gaussian(keys[4], (BLOCKS, D, D), D ** -0.5, 0.09375, ((1, 4), (2, 8))),
        "w_ingate": gaussian(keys[5], (BLOCKS, D, HEADS), D ** -0.5, 0.09375, ((1, 4),)),
        "w_forget": gaussian(keys[6], (BLOCKS, D, HEADS), D ** -0.5, 0.09375, ((1, 4),)),
        "forget_bias": jnp.clip(-2.0 + 5.0 * jax.random.uniform(keys[7], (BLOCKS, HEADS), jnp.float32) ** level_of(keys[7], (BLOCKS, HEADS), ((1, 8),), -0.2, 0.2), -2.0, 3.0),
        "head_gain": jnp.clip(1.0 + 0.18 * jax.random.normal(keys[8], (BLOCKS, HEADS, HEAD), jnp.float32), 0.1, 1.9),
        "w_proj": gaussian(keys[9], (BLOCKS, D, D), D ** -0.5, 0.09375, ((1, 8), (2, 4))),
        "mem_matrix": gaussian(keys[10], (BLOCKS, BATCH, HEADS, HEAD, HEAD), 0.1, 0.8, ((1, 4), (2, 8)), jnp.float32),
        "mem_norm": gaussian(keys[11], (BLOCKS, BATCH, HEADS, HEAD), 0.15, 1.2, ((1, 4), (2, 8)), jnp.float32),
        "mem_max": gaussian(keys[12], (BLOCKS, BATCH, HEADS), 1.0, 4.0, ((1, 4), (2, 8)), jnp.float32),
    }


norm_eps = 1e-06
head_eps = 1e-05

def full_sum(x_rows, weight):
    return jnp.dot(x_rows, weight, preferred_element_type=jnp.float32)

def cell_update(queries, key_vecs, values, log_in, log_forget, matrix, normvec, maxval):
    max_next = jnp.maximum(log_forget + maxval, log_in)
    decays = jnp.exp(log_forget + maxval - max_next)
    weight_in = jnp.exp(log_in - max_next)
    matrix_new = decays[..., None, None] * matrix + weight_in[..., None, None] * key_vecs[..., :, None] * values[..., None, :]
    norm_new = decays[..., None] * normvec + weight_in[..., None] * key_vecs
    numerator = jnp.einsum('bhd,bhde->bhe', queries, matrix_new, precision=lax.Precision.HIGHEST)
    denominator = jnp.maximum(jnp.abs(lax.optimization_barrier(jnp.sum(queries * norm_new, axis=-1))), 1.0)
    return (numerator / denominator[..., None], matrix_new, norm_new, max_next)

def head_norm(readout, gain, outgate):
    average = lax.optimization_barrier(jnp.mean(readout, axis=-1, keepdims=True))
    variance = lax.optimization_barrier(jnp.mean(jnp.square(readout - average), axis=-1, keepdims=True))
    normed = (readout - average) * lax.rsqrt(variance + head_eps) * gain
    return normed * jax.nn.sigmoid(outgate)

def mix_block(x_rows, weights, states):
    w_query, w_key, w_value, w_outgate, w_ingate, w_forget, bias, gain, w_proj = weights
    matrix, normvec, maxval = states
    row_count, features = x_rows.shape
    squares = lax.optimization_barrier(jnp.sum(jnp.square(x_rows.astype(jnp.float32)), axis=1))
    inv_scale = lax.rsqrt(squares / features + norm_eps)[:, None]
    head_shape = (row_count, HEADS, HEAD)
    queries = (full_sum(x_rows, w_query) * inv_scale).reshape(head_shape)
    key_vecs = (full_sum(x_rows, w_key) * inv_scale * HEAD ** (-0.5)).reshape(head_shape)
    values = (full_sum(x_rows, w_value) * inv_scale).reshape(head_shape)
    outgate = (full_sum(x_rows, w_outgate) * inv_scale).reshape(head_shape)
    log_in = full_sum(x_rows, w_ingate) * inv_scale
    log_forget = jax.nn.log_sigmoid(full_sum(x_rows, w_forget) * inv_scale + bias[None, :])
    readout, matrix_new, norm_new, max_next = cell_update(queries, key_vecs, values, log_in, log_forget, matrix, normvec, maxval)
    hidden = head_norm(readout, gain[None], outgate).reshape(row_count, -1).astype(jnp.bfloat16)
    mixed_out = jnp.dot(hidden, w_proj, preferred_element_type=jnp.float32).astype(jnp.bfloat16)
    return (mixed_out, matrix_new, norm_new, max_next)

def reference(tokens, w_query, w_key, w_value, w_outgate, w_ingate, w_forget, forget_bias, head_gain, w_proj, mem_matrix, mem_norm, mem_max):
    current = tokens
    matrix_list, norm_list, max_list = ([], [], [])
    for block_id in range(BLOCKS):
        weights = (w_query[block_id], w_key[block_id], w_value[block_id], w_outgate[block_id], w_ingate[block_id], w_forget[block_id], forget_bias[block_id], head_gain[block_id], w_proj[block_id])
        current, matrix_out, norm_out, max_out = mix_block(current, weights, (mem_matrix[block_id], mem_norm[block_id], mem_max[block_id]))
        matrix_list.append(matrix_out)
        norm_list.append(norm_out)
        max_list.append(max_out)
    return (current, jnp.stack(matrix_list), jnp.stack(norm_list), jnp.stack(max_list))
```

```python
import functools

import jax
import jax.numpy as jnp
from jax import lax
from jax.experimental import pallas as pl
from jax.experimental.pallas import tpu as pltpu
from jax.sharding import PartitionSpec as P

HEAD = 128
norm_eps = 1e-06
head_eps = 1e-05
MESH = pl.DeviceIdType.MESH
F32 = jnp.float32
BF16 = jnp.bfloat16
PART = F32
OUTP = F32
SPLIT = True


def chain_kernel(
    n_tp,
    n_dp,
    rows_tp,
    heads_all,
    tok_ref,
    wq_hbm,
    wk_hbm,
    wv_hbm,
    wo_hbm,
    wg_hbm,
    bias_ref,
    gain_ref,
    wp_hbm,
    mat_hbm,
    norm_ref,
    max_ref,
    res_ref,
    wkey_ref,
    val_ref,
    dec_ref,
    normo_ref,
    maxo_ref,
    w_vm,
    wg_vm,
    wp_vm,
    mat_vm,
    xbuf,
    psend,
    precv,
    gsend,
    grecv,
    hbuf,
    osend,
    orecv,
    q_scr,
    qm_scr,
    w_sem,
    wg_sem,
    wp_sem,
    mat_sem,
    x_ssem,
    x_rsem,
    p_ssem,
    p_rsem,
    g_ssem,
    g_rsem,
    h_ssem,
    h_rsem,
    o_ssem,
    o_rsem,
):
    tp = lax.axis_index("tp")
    dp = lax.axis_index("dp")
    cells = w_vm.shape[0]
    rp, feats = tok_ref.shape
    cols = w_vm.shape[3]
    heads = cols // HEAD
    rd = hbuf.shape[2]
    rows = n_tp * rp

    def load(src, dst, sem):
        return pltpu.make_async_copy(src, dst, sem)

    def loads(b):
        out = [load(wg_hbm.at[b], wg_vm.at[b], wg_sem.at[b])]
        for j, w in enumerate((wq_hbm, wk_hbm, wv_hbm, wo_hbm)):
            out.append(load(w.at[b], w_vm.at[b, j], w_sem.at[b, j]))
        out.append(load(mat_hbm.at[b], mat_vm.at[b], mat_sem.at[b]))
        out.append(load(wp_hbm.at[b], wp_vm.at[b], wp_sem.at[b]))
        return out

    for c in loads(0):
        c.start()

    barrier = pltpu.get_barrier_semaphore()
    for i in range(1, n_tp):
        pl.semaphore_signal(
            barrier, inc=1, device_id={"tp": lax.rem(tp + i, n_tp)}, device_id_type=MESH
        )
    for i in range(1, n_dp):
        pl.semaphore_signal(
            barrier, inc=1, device_id={"dp": lax.rem(dp + i, n_dp)}, device_id_type=MESH
        )
    xbuf[0, tp] = tok_ref[...]
    qm_scr[...] = jnp.zeros_like(qm_scr)
    for b in range(1, cells):
        for c in loads(b):
            c.start()
    pl.semaphore_wait(barrier, n_tp + n_dp - 2)

    def push(src, dst, ssem, rsem, axis, peer):
        return pltpu.make_async_remote_copy(
            src_ref=src,
            dst_ref=dst,
            send_sem=ssem,
            recv_sem=rsem,
            device_id={axis: peer},
            device_id_type=MESH,
        )

    def peers(me, n):
        return [(i, lax.rem(me + i, n), lax.rem(me + n - i, n)) for i in range(1, n)]

    lane = lax.broadcasted_iota(jnp.int32, (HEAD, cols), 1) // HEAD
    gate = lax.broadcasted_iota(jnp.int32, (HEAD, cols), 0)
    pick_in = (gate == tp * heads + lane).astype(F32)
    pick_forget = (gate == heads_all + tp * heads + lane).astype(F32)
    pick_square = (gate == 2 * heads_all).astype(F32)

    def exact(a, b):
        return jnp.dot(a, b, precision=lax.Precision.HIGHEST, preferred_element_type=F32)

    def cell(b, carry):
        sends = []
        for i, to, frm in peers(tp, n_tp):
            c = push(
                xbuf.at[b, tp], xbuf.at[b, tp], x_ssem.at[b, i], x_rsem.at[b, i], "tp", to
            )
            c.start()
            sends.append(c)
        for i, to, frm in peers(tp, n_tp):
            push(
                xbuf.at[b, frm], xbuf.at[b, frm], x_ssem.at[b, i], x_rsem.at[b, i], "tp", to
            ).wait_recv()
        x = xbuf[b].reshape(rows, feats)
        load(wg_hbm.at[b], wg_vm.at[b], wg_sem.at[b]).wait()
        xf = x.astype(F32)
        square = jnp.sum(xf * xf, axis=1, keepdims=True)
        gates = jnp.dot(x, wg_vm[b], preferred_element_type=F32)
        spot = lax.broadcasted_iota(jnp.int32, gates.shape, 1)
        gates = jnp.where(spot == 2 * heads_all, square, gates)
        gsend[b] = gates.reshape(n_dp, rd, HEAD)
        for i, to, frm in peers(dp, n_dp):
            c = push(
                gsend.at[b, to], grecv.at[b, dp], g_ssem.at[b, i], g_rsem.at[b, i], "dp", to
            )
            c.start()
            sends.append(c)
        for j, w in enumerate((wq_hbm, wk_hbm, wv_hbm, wo_hbm)):
            load(w.at[b], w_vm.at[b, j], w_sem.at[b, j]).wait()
            part = jnp.dot(x, w_vm[b, j], preferred_element_type=F32)
            psend[b, j] = part.astype(PART).reshape(n_dp, rd, cols)
            for i, to, frm in peers(dp, n_dp):
                c = push(
                    psend.at[b, j, to],
                    precv.at[b, j, dp],
                    p_ssem.at[b, j, i],
                    p_rsem.at[b, j, i],
                    "dp",
                    to,
                )
                c.start()
                sends.append(c)
        for i, to, frm in peers(dp, n_dp):
            push(
                gsend.at[b, to], grecv.at[b, frm], g_ssem.at[b, i], g_rsem.at[b, i], "dp", to
            ).wait_recv()
        total = gsend[b, dp]
        for i, to, frm in peers(dp, n_dp):
            total = total + grecv[b, frm]
        squares = exact(total, pick_square)
        inv = lax.rsqrt(squares / (feats * n_dp) + norm_eps)
        log_in = exact(total, pick_in) * inv
        raw = exact(total, pick_forget) * inv + bias_ref[b]
        log_forget = jnp.minimum(raw, 0.0) - jnp.log1p(jnp.exp(-jnp.abs(raw)))
        held = log_forget + max_ref[b]
        max_next = jnp.maximum(held, log_in)
        decays = jnp.exp(held - max_next)
        weight_in = jnp.exp(log_in - max_next)

        def summed(j):
            for i, to, frm in peers(dp, n_dp):
                push(
                    psend.at[b, j, to],
                    precv.at[b, j, frm],
                    p_ssem.at[b, j, i],
                    p_rsem.at[b, j, i],
                    "dp",
                    to,
                ).wait_recv()
            acc = psend[b, j, dp].astype(F32)
            for i, to, frm in peers(dp, n_dp):
                acc = acc + precv[b, j, frm].astype(F32)
            return acc * inv

        query = summed(0)
        for h in range(heads):
            q_scr[h] = query[:, h * HEAD : (h + 1) * HEAD]
        load(mat_hbm.at[b], mat_vm.at[b], mat_sem.at[b]).wait()

        group = 7 if rows_tp % 7 == 0 else 1
        per = rows_tp // group

        first = lax.broadcasted_iota(jnp.int32, (16, HEAD), 0) == 0

        def read(step, carry):
            base = (step // per) * rp + lax.rem(step, per) * group
            for s in range(group):
                for h in range(heads):
                    row = q_scr[h, pl.ds(base + s, 1), :]
                    spread = jnp.broadcast_to(row, (16, HEAD))
                    high = spread.astype(BF16).astype(F32)
                    lhs = jnp.where(first, high, spread - high).astype(BF16)
                    m = mat_vm[b, step * group + s, h]
                    top = m.astype(BF16)
                    got = jnp.dot(lhs, top, preferred_element_type=F32)
                    if SPLIT:
                        rest = (m - top.astype(F32)).astype(BF16)
                        got = got + jnp.dot(lhs, rest, preferred_element_type=F32)
                    qm_scr[h, pl.ds(base + s, 1), :] = got[0:1] + got[1:2]
            return carry

        lax.fori_loop(0, mat_vm.shape[1] // group, read, 0)

        wkey = summed(1) * (HEAD**-0.5) * weight_in
        value = summed(2)
        outgate = summed(3)
        norm_new = decays * norm_ref[b] + wkey
        wkey_ref[b] = wkey
        val_ref[b] = value
        dec_ref[b] = decays
        normo_ref[b] = norm_new
        maxo_ref[b] = max_next
        for h in range(heads):
            at = slice(h * HEAD, (h + 1) * HEAD)
            qh = query[:, at]
            dot_n = jnp.sum(qh * norm_new[:, at], axis=1, keepdims=True)
            dot_k = jnp.sum(qh * wkey[:, at], axis=1, keepdims=True)
            top = decays[:, at] * qm_scr[h] + dot_k * value[:, at]
            readout = top / jnp.maximum(jnp.abs(dot_n), 1.0)
            average = jnp.mean(readout, axis=1, keepdims=True)
            away = readout - average
            variance = jnp.mean(away * away, axis=1, keepdims=True)
            normed = away * lax.rsqrt(variance + head_eps) * gain_ref[b][:, at]
            hidden = normed * jax.nn.sigmoid(outgate[:, at])
            hbuf[b, dp, :, at] = hidden.astype(BF16)
        for i, to, frm in peers(dp, n_dp):
            c = push(
                hbuf.at[b, dp], hbuf.at[b, dp], h_ssem.at[b, i], h_rsem.at[b, i], "dp", to
            )
            c.start()
            sends.append(c)
        load(wp_hbm.at[b], wp_vm.at[b], wp_sem.at[b]).wait()
        for i, to, frm in peers(dp, n_dp):
            push(
                hbuf.at[b, frm], hbuf.at[b, frm], h_ssem.at[b, i], h_rsem.at[b, i], "dp", to
            ).wait_recv()
        full = hbuf[b].reshape(rows, cols)
        out = jnp.dot(full, wp_vm[b], preferred_element_type=F32)
        osend[b] = out.astype(OUTP).reshape(n_tp, rp, feats)
        for i, to, frm in peers(tp, n_tp):
            c = push(
                osend.at[b, to], orecv.at[b, tp], o_ssem.at[b, i], o_rsem.at[b, i], "tp", to
            )
            c.start()
            sends.append(c)
        for i, to, frm in peers(tp, n_tp):
            push(
                osend.at[b, to], orecv.at[b, frm], o_ssem.at[b, i], o_rsem.at[b, i], "tp", to
            ).wait_recv()
        acc = osend[b, tp].astype(F32)
        for i, to, frm in peers(tp, n_tp):
            acc = acc + orecv[b, frm].astype(F32)
        xbuf[b + 1, tp] = acc.astype(BF16)
        for c in sends:
            c.wait_send()
        return carry

    lax.fori_loop(0, cells, cell, 0)
    res_ref[...] = xbuf[cells, tp]


def on_device(
    tokens,
    w_query,
    w_key,
    w_value,
    w_outgate,
    w_ingate,
    w_forget,
    forget_bias,
    head_gain,
    w_proj,
    mem_matrix,
    mem_norm,
    mem_max,
):
    n_tp, n_dp = lax.axis_size("tp"), lax.axis_size("dp")
    rows_tp, feats = tokens.shape
    rp = -(-rows_tp // 16) * 16
    cells, _, cols = w_query.shape
    seqs, heads = mem_max.shape[1:]
    blocks = seqs // rows_tp
    rd = blocks * rp
    heads_all = w_ingate.shape[2]
    more = rp - rows_tp

    def padded(a):
        a = a.reshape(cells, blocks, rows_tp, cols)
        return jnp.pad(a, ((0, 0), (0, 0), (0, more), (0, 0))).reshape(cells, rd, cols)

    def compact(a):
        a = a.reshape(cells, blocks, rp, heads, HEAD)[:, :, :rows_tp]
        return a.reshape(cells, seqs, heads, HEAD)

    def spread(a):
        return jnp.broadcast_to(a[..., None], a.shape + (HEAD,))

    toks = jnp.pad(tokens, ((0, more), (0, 0)))
    w_gate = jnp.concatenate([w_ingate, w_forget], axis=2)
    w_gate = jnp.pad(w_gate, ((0, 0), (0, 0), (0, HEAD - 2 * heads_all)))
    bias = spread(forget_bias).reshape(cells, 1, cols)
    gain = head_gain.reshape(cells, 1, cols)
    norm_in = padded(mem_norm)
    max_in = padded(spread(mem_max))

    vm = pl.BlockSpec(memory_space=pltpu.VMEM)
    hbm = pl.BlockSpec(memory_space=pl.ANY)
    dma = pltpu.SemaphoreType.DMA
    state = jax.ShapeDtypeStruct((cells, rd, cols), F32)
    result, wkey, value, decays, norm_new, max_new = pl.pallas_call(
        functools.partial(chain_kernel, n_tp, n_dp, rows_tp, heads_all),
        out_shape=(jax.ShapeDtypeStruct((rp, feats), BF16),) + (state,) * 5,
        in_specs=[vm, hbm, hbm, hbm, hbm, hbm, vm, vm, hbm, hbm, vm, vm],
        out_specs=(vm,) * 6,
        scratch_shapes=[
            pltpu.VMEM((cells, 4, feats, cols), BF16),
            pltpu.VMEM((cells, feats, HEAD), BF16),
            pltpu.VMEM((cells,) + w_proj.shape[1:], BF16),
            pltpu.VMEM(mem_matrix.shape, F32),
            pltpu.VMEM((cells + 1, n_tp, rp, feats), BF16),
            pltpu.VMEM((cells, 4, n_dp, rd, cols), PART),
            pltpu.VMEM((cells, 4, n_dp, rd, cols), PART),
            pltpu.VMEM((cells, n_dp, rd, HEAD), F32),
            pltpu.VMEM((cells, n_dp, rd, HEAD), F32),
            pltpu.VMEM((cells, n_dp, rd, cols), BF16),
            pltpu.VMEM((cells, n_tp, rp, feats), OUTP),
            pltpu.VMEM((cells, n_tp, rp, feats), OUTP),
            pltpu.VMEM((heads, rd, HEAD), F32),
            pltpu.VMEM((heads, rd, HEAD), F32),
            dma((cells, 4)),
            dma((cells,)),
            dma((cells,)),
            dma((cells,)),
            dma((cells, n_tp)),
            dma((cells, n_tp)),
            dma((cells, 4, n_dp)),
            dma((cells, 4, n_dp)),
            dma((cells, n_dp)),
            dma((cells, n_dp)),
            dma((cells, n_dp)),
            dma((cells, n_dp)),
            dma((cells, n_tp)),
            dma((cells, n_tp)),
        ],
        compiler_params=pltpu.CompilerParams(
            collective_id=0, has_side_effects=True, vmem_limit_bytes=56 * 2**20
        ),
    )(
        toks,
        w_query,
        w_key,
        w_value,
        w_outgate,
        w_gate,
        bias,
        gain,
        w_proj,
        mem_matrix,
        norm_in,
        max_in,
    )
    key_vecs = compact(wkey)
    values = compact(value)
    decay = compact(decays)[..., :1]
    matrix_new = decay[..., None] * mem_matrix + key_vecs[..., :, None] * values[..., None, :]
    return (result[:rows_tp], matrix_new, compact(norm_new), compact(max_new)[..., 0])


def solution(mesh):
    in_specs = (
        P("tp", "dp"),
        P(None, "dp", "tp"),
        P(None, "dp", "tp"),
        P(None, "dp", "tp"),
        P(None, "dp", "tp"),
        P(None, "dp", None),
        P(None, "dp", None),
        P(None, "tp"),
        P(None, "tp", None),
        P(None, "tp", "dp"),
        P(None, "dp", "tp", None, None),
        P(None, "dp", "tp", None),
        P(None, "dp", "tp"),
    )
    out_specs = (
        P("tp", "dp"),
        P(None, "dp", "tp", None, None),
        P(None, "dp", "tp", None),
        P(None, "dp", "tp"),
    )
    return jax.shard_map(
        on_device, mesh=mesh, in_specs=in_specs, out_specs=out_specs, check_vma=False
    )
```

```python
import functools

import jax
import jax.numpy as jnp
from jax import lax
from jax.experimental import pallas as pl
from jax.experimental.pallas import tpu as pltpu
from jax.sharding import PartitionSpec as P

HEAD = 128
norm_eps = 1e-06
head_eps = 1e-05
MESH = pl.DeviceIdType.MESH
F32 = jnp.float32
BF16 = jnp.bfloat16
PART = F32
OUTP = F32
SPLIT = True


def chain_kernel(
    n_tp,
    n_dp,
    rows_tp,
    heads_all,
    tok_ref,
    wq_hbm,
    wk_hbm,
    wv_hbm,
    wo_hbm,
    wi_hbm,
    wf_hbm,
    bias_ref,
    gain_ref,
    wp_hbm,
    mat_hbm,
    norm_ref,
    max_ref,
    res_ref,
    wkey_ref,
    val_ref,
    dec_ref,
    normo_ref,
    maxo_ref,
    w_vm,
    wg_vm,
    wp_vm,
    mat_vm,
    xbuf,
    psend,
    precv,
    gsend,
    grecv,
    hbuf,
    osend,
    orecv,
    q_scr,
    qm_scr,
    w_sem,
    wg_sem,
    wp_sem,
    mat_sem,
    x_ssem,
    x_rsem,
    p_ssem,
    p_rsem,
    g_ssem,
    g_rsem,
    h_ssem,
    h_rsem,
    o_ssem,
    o_rsem,
):
    tp = lax.axis_index("tp")
    dp = lax.axis_index("dp")
    cells = w_vm.shape[0]
    rp, feats = xbuf.shape[2:]
    cols = w_vm.shape[3]
    heads = cols // HEAD
    rd = hbuf.shape[2]
    rows = n_tp * rp

    def load(src, dst, sem):
        return pltpu.make_async_copy(src, dst, sem)

    def gate_loads(b):
        low, high = pl.ds(0, heads_all), pl.ds(heads_all, heads_all)
        return [
            load(wi_hbm.at[b], wg_vm.at[b, low], wg_sem.at[b, 0]),
            load(wf_hbm.at[b], wg_vm.at[b, high], wg_sem.at[b, 1]),
        ]

    def loads(b):
        out = gate_loads(b)
        for j, w in enumerate((wq_hbm, wk_hbm, wv_hbm, wo_hbm)):
            out.append(load(w.at[b], w_vm.at[b, j], w_sem.at[b, j]))
        out.append(load(mat_hbm.at[b], mat_vm.at[b], mat_sem.at[b]))
        out.append(load(wp_hbm.at[b], wp_vm.at[b], wp_sem.at[b]))
        return out

    for c in loads(0):
        c.start()

    barrier = pltpu.get_barrier_semaphore()
    for i in range(1, n_tp):
        pl.semaphore_signal(
            barrier, inc=1, device_id={"tp": lax.rem(tp + i, n_tp)}, device_id_type=MESH
        )
    for i in range(1, n_dp):
        pl.semaphore_signal(
            barrier, inc=1, device_id={"dp": lax.rem(dp + i, n_dp)}, device_id_type=MESH
        )
    xbuf[0, tp] = jnp.zeros((rp, feats), BF16)
    xbuf[0, tp, :rows_tp] = tok_ref[...]
    wg_vm[:, 2 * heads_all :] = jnp.zeros((cells, HEAD - 2 * heads_all, feats), BF16)
    qm_scr[...] = jnp.zeros_like(qm_scr)
    for b in range(1, cells):
        for c in loads(b):
            c.start()
    pl.semaphore_wait(barrier, n_tp + n_dp - 2)

    def push(src, dst, ssem, rsem, axis, peer):
        return pltpu.make_async_remote_copy(
            src_ref=src,
            dst_ref=dst,
            send_sem=ssem,
            recv_sem=rsem,
            device_id={axis: peer},
            device_id_type=MESH,
        )

    def peers(me, n):
        return [(i, lax.rem(me + i, n), lax.rem(me + n - i, n)) for i in range(1, n)]

    lane = lax.broadcasted_iota(jnp.int32, (HEAD, cols), 1) // HEAD
    gate = lax.broadcasted_iota(jnp.int32, (HEAD, cols), 0)
    pick_in = (gate == tp * heads + lane).astype(F32)
    pick_forget = (gate == heads_all + tp * heads + lane).astype(F32)
    pick_square = (gate == 2 * heads_all).astype(F32)

    def exact(a, b):
        return jnp.dot(a, b, precision=lax.Precision.HIGHEST, preferred_element_type=F32)

    def cell(b, carry):
        sends = []
        for i, to, frm in peers(tp, n_tp):
            c = push(
                xbuf.at[b, tp], xbuf.at[b, tp], x_ssem.at[b, i], x_rsem.at[b, i], "tp", to
            )
            c.start()
            sends.append(c)
        for i, to, frm in peers(tp, n_tp):
            push(
                xbuf.at[b, frm], xbuf.at[b, frm], x_ssem.at[b, i], x_rsem.at[b, i], "tp", to
            ).wait_recv()
        x = xbuf[b].reshape(rows, feats)
        for c in gate_loads(b):
            c.wait()
        xf = x.astype(F32)
        square = jnp.sum(xf * xf, axis=1, keepdims=True)
        gates = lax.dot_general(
            x, wg_vm[b], (((1,), (1,)), ((), ())), preferred_element_type=F32
        )
        spot = lax.broadcasted_iota(jnp.int32, gates.shape, 1)
        gates = jnp.where(spot == 2 * heads_all, square, gates)
        gsend[b] = gates.reshape(n_dp, rd, HEAD)
        for i, to, frm in peers(dp, n_dp):
            c = push(
                gsend.at[b, to], grecv.at[b, dp], g_ssem.at[b, i], g_rsem.at[b, i], "dp", to
            )
            c.start()
            sends.append(c)
        for j, w in enumerate((wq_hbm, wk_hbm, wv_hbm, wo_hbm)):
            load(w.at[b], w_vm.at[b, j], w_sem.at[b, j]).wait()
            part = jnp.dot(x, w_vm[b, j], preferred_element_type=F32)
            psend[b, j] = part.astype(PART).reshape(n_dp, rd, cols)
            for i, to, frm in peers(dp, n_dp):
                c = push(
                    psend.at[b, j, to],
                    precv.at[b, j, dp],
                    p_ssem.at[b, j, i],
                    p_rsem.at[b, j, i],
                    "dp",
                    to,
                )
                c.start()
                sends.append(c)
        for i, to, frm in peers(dp, n_dp):
            push(
                gsend.at[b, to], grecv.at[b, frm], g_ssem.at[b, i], g_rsem.at[b, i], "dp", to
            ).wait_recv()
        total = gsend[b, dp]
        for i, to, frm in peers(dp, n_dp):
            total = total + grecv[b, frm]
        squares = exact(total, pick_square)
        inv = lax.rsqrt(squares / (feats * n_dp) + norm_eps)
        log_in = exact(total, pick_in) * inv
        raw = exact(total, pick_forget) * inv + bias_ref[b]
        log_forget = jnp.minimum(raw, 0.0) - jnp.log1p(jnp.exp(-jnp.abs(raw)))
        held = log_forget + max_ref[b]
        max_next = jnp.maximum(held, log_in)
        decays = jnp.exp(held - max_next)
        weight_in = jnp.exp(log_in - max_next)

        def summed(j):
            for i, to, frm in peers(dp, n_dp):
                push(
                    psend.at[b, j, to],
                    precv.at[b, j, frm],
                    p_ssem.at[b, j, i],
                    p_rsem.at[b, j, i],
                    "dp",
                    to,
                ).wait_recv()
            acc = psend[b, j, dp].astype(F32)
            for i, to, frm in peers(dp, n_dp):
                acc = acc + precv[b, j, frm].astype(F32)
            return acc * inv

        query = summed(0)
        for h in range(heads):
            q_scr[h] = query[:, h * HEAD : (h + 1) * HEAD]
        load(mat_hbm.at[b], mat_vm.at[b], mat_sem.at[b]).wait()

        group = 7 if rows_tp % 7 == 0 else 1
        per = rows_tp // group

        first = lax.broadcasted_iota(jnp.int32, (16, HEAD), 0) == 0

        def read(step, carry):
            base = (step // per) * rp + lax.rem(step, per) * group
            for s in range(group):
                for h in range(heads):
                    row = q_scr[h, pl.ds(base + s, 1), :]
                    spread = jnp.broadcast_to(row, (16, HEAD))
                    high = spread.astype(BF16).astype(F32)
                    lhs = jnp.where(first, high, spread - high).astype(BF16)
                    m = mat_vm[b, step * group + s, h]
                    top = m.astype(BF16)
                    got = jnp.dot(lhs, top, preferred_element_type=F32)
                    if SPLIT:
                        rest = (m - top.astype(F32)).astype(BF16)
                        got = got + jnp.dot(lhs, rest, preferred_element_type=F32)
                    qm_scr[h, pl.ds(base + s, 1), :] = got[0:1] + got[1:2]
            return carry

        lax.fori_loop(0, mat_vm.shape[1] // group, read, 0)

        wkey = summed(1) * (HEAD**-0.5) * weight_in
        value = summed(2)
        outgate = summed(3)
        norm_new = decays * norm_ref[b] + wkey
        wkey_ref[b] = wkey
        val_ref[b] = value
        dec_ref[b] = decays
        normo_ref[b] = norm_new
        maxo_ref[b] = max_next
        for h in range(heads):
            at = slice(h * HEAD, (h + 1) * HEAD)
            qh = query[:, at]
            dot_n = jnp.sum(qh * norm_new[:, at], axis=1, keepdims=True)
            dot_k = jnp.sum(qh * wkey[:, at], axis=1, keepdims=True)
            top = decays[:, at] * qm_scr[h] + dot_k * value[:, at]
            readout = top / jnp.maximum(jnp.abs(dot_n), 1.0)
            average = jnp.mean(readout, axis=1, keepdims=True)
            away = readout - average
            variance = jnp.mean(away * away, axis=1, keepdims=True)
            normed = away * lax.rsqrt(variance + head_eps) * gain_ref[b][:, at]
            hidden = normed * jax.nn.sigmoid(outgate[:, at])
            hbuf[b, dp, :, at] = hidden.astype(BF16)
        for i, to, frm in peers(dp, n_dp):
            c = push(
                hbuf.at[b, dp], hbuf.at[b, dp], h_ssem.at[b, i], h_rsem.at[b, i], "dp", to
            )
            c.start()
            sends.append(c)
        load(wp_hbm.at[b], wp_vm.at[b], wp_sem.at[b]).wait()
        for i, to, frm in peers(dp, n_dp):
            push(
                hbuf.at[b, frm], hbuf.at[b, frm], h_ssem.at[b, i], h_rsem.at[b, i], "dp", to
            ).wait_recv()
        full = hbuf[b].reshape(rows, cols)
        out = jnp.dot(full, wp_vm[b], preferred_element_type=F32)
        osend[b] = out.astype(OUTP).reshape(n_tp, rp, feats)
        for i, to, frm in peers(tp, n_tp):
            c = push(
                osend.at[b, to], orecv.at[b, tp], o_ssem.at[b, i], o_rsem.at[b, i], "tp", to
            )
            c.start()
            sends.append(c)
        for i, to, frm in peers(tp, n_tp):
            push(
                osend.at[b, to], orecv.at[b, frm], o_ssem.at[b, i], o_rsem.at[b, i], "tp", to
            ).wait_recv()
        acc = osend[b, tp].astype(F32)
        for i, to, frm in peers(tp, n_tp):
            acc = acc + orecv[b, frm].astype(F32)
        xbuf[b + 1, tp] = acc.astype(BF16)
        for c in sends:
            c.wait_send()
        return carry

    lax.fori_loop(0, cells, cell, 0)
    res_ref[...] = xbuf[cells, tp]


def on_device(
    tokens,
    w_query,
    w_key,
    w_value,
    w_outgate,
    w_ingate,
    w_forget,
    forget_bias,
    head_gain,
    w_proj,
    mem_matrix,
    mem_norm,
    mem_max,
):
    n_tp, n_dp = lax.axis_size("tp"), lax.axis_size("dp")
    rows_tp, feats = tokens.shape
    rp = -(-rows_tp // 16) * 16
    cells, _, cols = w_query.shape
    seqs, heads = mem_max.shape[1:]
    blocks = seqs // rows_tp
    rd = blocks * rp
    heads_all = w_ingate.shape[2]
    more = rp - rows_tp

    def padded(a):
        a = a.reshape(cells, blocks, rows_tp, cols)
        return jnp.pad(a, ((0, 0), (0, 0), (0, more), (0, 0))).reshape(cells, rd, cols)

    def compact(a):
        a = a.reshape(cells, blocks, rp, heads, HEAD)[:, :, :rows_tp]
        return a.reshape(cells, seqs, heads, HEAD)

    def spread(a):
        return jnp.broadcast_to(a[..., None], a.shape + (HEAD,))

    w_in, w_fg = jnp.swapaxes(w_ingate, 1, 2), jnp.swapaxes(w_forget, 1, 2)
    bias = spread(forget_bias).reshape(cells, 1, cols)
    gain = head_gain.reshape(cells, 1, cols)
    norm_in = padded(mem_norm)
    max_in = padded(spread(mem_max))

    vm = pl.BlockSpec(memory_space=pltpu.VMEM)
    hbm = pl.BlockSpec(memory_space=pl.ANY)
    dma = pltpu.SemaphoreType.DMA
    state = jax.ShapeDtypeStruct((cells, rd, cols), F32)
    result, wkey, value, decays, norm_new, max_new = pl.pallas_call(
        functools.partial(chain_kernel, n_tp, n_dp, rows_tp, heads_all),
        out_shape=(jax.ShapeDtypeStruct((rp, feats), BF16),) + (state,) * 5,
        in_specs=[vm, hbm, hbm, hbm, hbm, hbm, hbm, vm, vm, hbm, hbm, vm, vm],
        out_specs=(vm,) * 6,
        scratch_shapes=[
            pltpu.VMEM((cells, 4, feats, cols), BF16),
            pltpu.VMEM((cells, HEAD, feats), BF16),
            pltpu.VMEM((cells,) + w_proj.shape[1:], BF16),
            pltpu.VMEM(mem_matrix.shape, F32),
            pltpu.VMEM((cells + 1, n_tp, rp, feats), BF16),
            pltpu.VMEM((cells, 4, n_dp, rd, cols), PART),
            pltpu.VMEM((cells, 4, n_dp, rd, cols), PART),
            pltpu.VMEM((cells, n_dp, rd, HEAD), F32),
            pltpu.VMEM((cells, n_dp, rd, HEAD), F32),
            pltpu.VMEM((cells, n_dp, rd, cols), BF16),
            pltpu.VMEM((cells, n_tp, rp, feats), OUTP),
            pltpu.VMEM((cells, n_tp, rp, feats), OUTP),
            pltpu.VMEM((heads, rd, HEAD), F32),
            pltpu.VMEM((heads, rd, HEAD), F32),
            dma((cells, 4)),
            dma((cells, 2)),
            dma((cells,)),
            dma((cells,)),
            dma((cells, n_tp)),
            dma((cells, n_tp)),
            dma((cells, 4, n_dp)),
            dma((cells, 4, n_dp)),
            dma((cells, n_dp)),
            dma((cells, n_dp)),
            dma((cells, n_dp)),
            dma((cells, n_dp)),
            dma((cells, n_tp)),
            dma((cells, n_tp)),
        ],
        compiler_params=pltpu.CompilerParams(
            collective_id=0, has_side_effects=True, vmem_limit_bytes=56 * 2**20
        ),
    )(
        tokens,
        w_query,
        w_key,
        w_value,
        w_outgate,
        w_in,
        w_fg,
        bias,
        gain,
        w_proj,
        mem_matrix,
        norm_in,
        max_in,
    )
    key_vecs = compact(wkey)
    values = compact(value)
    decay = compact(decays)[..., :1]
    matrix_new = decay[..., None] * mem_matrix + key_vecs[..., :, None] * values[..., None, :]
    return (result[:rows_tp], matrix_new, compact(norm_new), compact(max_new)[..., 0])


def solution(mesh):
    in_specs = (
        P("tp", "dp"),
        P(None, "dp", "tp"),
        P(None, "dp", "tp"),
        P(None, "dp", "tp"),
        P(None, "dp", "tp"),
        P(None, "dp", None),
        P(None, "dp", None),
        P(None, "tp"),
        P(None, "tp", None),
        P(None, "tp", "dp"),
        P(None, "dp", "tp", None, None),
        P(None, "dp", "tp", None),
        P(None, "dp", "tp"),
    )
    out_specs = (
        P("tp", "dp"),
        P(None, "dp", "tp", None, None),
        P(None, "dp", "tp", None),
        P(None, "dp", "tp"),
    )
    return jax.shard_map(
        on_device, mesh=mesh, in_specs=in_specs, out_specs=out_specs, check_vma=False
    )
```
